32 devices in a mesh: ep: 8 (over z, core), tp: 4 (over y, x).
Axes of the slice: x: 2, y: 2, z: 4, core: 2. Of those that a mesh axis runs over, the one named last changes fastest.
Arguments:
- mixer_input: bfloat16 [2048, 2048], P('ep'), may hold values from -6 to 6
- mixer_gain: float32 [2048], replicated, may hold values from 0.1 to 1.9
- query_weight: bfloat16 [2048, 2048], P(None, 'tp'), may hold values from -0.13258252 to 0.13258252
- key_weight: bfloat16 [2048, 1024], P(None, 'tp'), may hold values from -2.78423295 to 2.78423295
- value_weight: bfloat16 [2048, 1024], P(None, 'tp'), may hold values from -0.125 to 0.125
- output_weight: bfloat16 [2048, 2048], P(None, 'tp'), may hold values from -1 to 1
- sink_logit: float32 [32], P('tp'), may hold values from 2 to 7
- expert_input: bfloat16 [1024, 2048], P('ep'), may hold values from -6 to 6
- expert_gain: float32 [2048], replicated, may hold values from 0.1 to 1.9
- routes: int32 [1024, 4], P('ep'), may hold values from 0 to 7, all different within a row; in each aligned block of 128 rows (0 to 127, 128 to 255, ...) at most 128 rows name the same one
- route_logits: float32 [1024, 4], P('ep'), may hold values from -6 to 6
- gate_weight: bfloat16 [8, 2048, 2048], P('ep', None, 'tp'), may hold values from -0.375 to 0.375
- up_weight: bfloat16 [8, 2048, 2048], P('ep', None, 'tp'), may hold values from -0.375 to 0.375
- down_weight: bfloat16 [8, 2048, 2048], P('ep', None, 'tp'), may hold values from -0.03125 to 0.03125
Outputs:
- mixer_output: bfloat16 [2048, 2048], P('ep', 'tp')
- expert_output: bfloat16 [1024, 2048], P('ep', 'tp')
The draws below stay inside these ranges and needn't reach their ends.
Inputs may be any that keep to these rules, and one draw needn't show every extreme that they name: `routes`: each token names 4 different experts. Among the 128 tokens of one index of ep (aligned blocks) no expert is named more than 128 times, and in some blocks one expert is named exactly 128 times.
All inputs are finite; a program needn't handle non-finite values.
Results may differ from the reference program's by a relative error of at most 0.0055.
The reference program's roundings to bfloat16 on the way count: a program that leaves them out, or rounds other values in their place, can miss the bound.
Values may be sent and summed in bfloat16 or wider, within the bound.
A program may use at most 64 MiB of HBM per device.

```python
import math
import jax
import jax.numpy as jnp
import numpy as np
from jax import lax

D = 2048
HEADS = 32
KV_HEADS = 16
HEAD_DIM = 64
FF = 2048
TOP_K = 4
WINDOW = 128
GRID_W = 64
EXP_DEV = 128
EXPERTS = 8
CAP = 128
MIX_TOKENS = 2048
EXP_TOKENS = 1024
N_EP = 8


def paired_weights(key):
    base = jax.random.fold_in(key, 11)
    first, second = jax.random.split(base)
    query = jnp.clip(jax.random.normal(first, (D, HEADS * HEAD_DIM), jnp.float32), -6.0, 6.0) / math.sqrt(D)
    noise = jnp.clip(jax.random.normal(second, (D, KV_HEADS * HEAD_DIM), jnp.float32), -6.0, 6.0) / math.sqrt(D)
    keys = noise
    return (query, keys)


def draw_query_weight(key, part):
    return paired_weights(key)[0].astype(jnp.bfloat16)


def draw_key_weight(key, part):
    return paired_weights(key)[1].astype(jnp.bfloat16)


def levels(rng, shape, pieces, least, largest):
    level = 1.0
    for position, blocks in pieces:
        draws = jax.random.uniform(jax.random.fold_in(jax.random.fold_in(rng, 6), position), (blocks,), jnp.float32, least / len(pieces), largest / len(pieces))
        level = level * jnp.repeat(jnp.exp(draws), shape[position] // blocks).reshape((-1,) + (1,) * (len(shape) - 1 - position))
    return level


def routed_block(own_key, own, number, rows, amount, top, reach, slope):
    sequence = jax.random.permutation(own_key, amount)
    packed, common = portions_of(amount, rows * top, reach, slope, True), portions_of(amount, rows * top, reach, slope, False)
    places = jnp.arange(amount)

    def named(sizes, rotation):
        used = int((sizes > 0).sum())
        fixed = max(1, used // 4)
        moved = fixed + (places - fixed + rotation * (used - fixed)) % max(1, amount - fixed)
        return jnp.zeros((amount,), jnp.int32).at[sequence[jnp.where(places < fixed, places, moved)]].set(jnp.asarray(sizes, jnp.int32))

    sizes = jnp.where(number % 4 == 0, named(packed, number // 4), named(common, number - number // 4 - 1))
    mixed = jax.random.permutation(jax.random.fold_in(own, 3), amount)
    giver, sink = mixed[0:amount // 2 * 2:2], mixed[1:amount // 2 * 2:2]
    margin = jnp.minimum(sizes[giver] - 1, reach - sizes[sink]) // 2
    margin = jnp.where((giver == sequence[0]) | (sink == sequence[0]) | (sizes[sink] == 0), 0, jnp.maximum(margin, 0))
    moved = jax.random.randint(jax.random.fold_in(own, 4), (amount // 2,), 0, 1 << 20) % (margin + 1)
    sizes = sizes.at[giver].add(-moved).at[sink].add(moved)
    labels = jnp.searchsorted(jnp.cumsum(sizes), jnp.arange(rows * top), side="right").astype(jnp.int32)
    grid = labels.reshape(top, rows).T
    grid = grid[jax.random.permutation(jax.random.fold_in(own, 1), rows)]
    rotation = jax.random.randint(jax.random.fold_in(own, 2), (rows, 1), 0, top)
    return jnp.take_along_axis(grid, (jnp.arange(top)[None, :] + rotation) % top, axis=1)


def portions_of(amount, total, reach, slope, full):
    portions = [(1 << 20) // math.isqrt(standing ** slope) + 1 for standing in range(1, amount + 1)]
    largest = reach if full else min(reach, max(-(-total // amount), total * portions[0] // sum(portions)))
    least = 1 if total - largest >= amount - 1 else 0
    given, rest = [largest] + [least] * (amount - 1), total - largest - least * (amount - 1)
    while rest > 0:
        free = [i for i in range(1, amount) if given[i] < largest] or [i for i in range(1, amount) if given[i] < reach]
        whole, remaining = sum([portions[i] for i in free]), rest
        for i in free:
            addition = min(reach - given[i], max(1, remaining * portions[i] // whole), rest)
            given[i] = given[i] + addition
            rest = rest - addition
    return np.array(given)


def gaussian(rng, extent, width, reach, cuts=(), kind=jnp.bfloat16):
    entries = jax.random.normal(rng, extent, jnp.float32) * width
    if len(cuts) > 0:
        entries = levels(rng, extent, cuts, -0.22, 0.18) * entries
    return jnp.clip(entries, min=-reach, max=reach).astype(kind)


def setup_inputs(seed: int = 0) -> dict:
    splits = jax.random.split(jax.random.key(seed), 15)
    mixer_input = gaussian(splits[0], (MIX_TOKENS, D), 1.0, 6.0, ((0, 8),))
    mixer_gain = jnp.clip(1.0 + 0.18 * jax.random.normal(splits[1], (D,), jnp.float32), 0.1, 1.9)
    query_weight = draw_query_weight(jax.random.fold_in(splits[14], 71), 0)
    key_weight = draw_key_weight(jax.random.fold_in(splits[14], 71), 0)
    value_weight = gaussian(splits[4], (D, KV_HEADS * HEAD_DIM), D ** -0.5, 0.125, ((1, 4),))
    output_weight = gaussian(splits[5], (HEADS * HEAD_DIM, D), (HEADS * HEAD_DIM // 64) ** -0.5, 1.0, ((1, 4),))
    sink_logit = jnp.clip(2.0 + 5.0 * jax.random.uniform(splits[6], (HEADS,), jnp.float32) ** levels(splits[6], (HEADS,), ((0, 4),), -0.2, 0.2), 2.0, 7.0)
    expert_input = gaussian(splits[7], (EXP_TOKENS, D), 1.0, 6.0, ((0, 8),))
    expert_gain = jnp.clip(1.0 + 0.18 * jax.random.normal(splits[8], (D,), jnp.float32), 0.1, 1.9)
    routes_keys = jax.random.split(jax.random.fold_in(splits[9], 1), EXP_TOKENS // EXP_DEV)
    routes_turns = jax.random.permutation(jax.random.fold_in(splits[9], 3), EXP_TOKENS // EXP_DEV)
    routes = jax.vmap(lambda own, number: routed_block(jax.random.fold_in(splits[9], 2), own, number, EXP_DEV, EXPERTS, TOP_K, CAP, 2))(routes_keys, routes_turns).reshape((EXP_TOKENS, TOP_K))
    route_logits = gaussian(splits[10], (EXP_TOKENS, TOP_K), 1.5, 6.0, ((0, 8),), jnp.float32)
    gate_weight = gaussian(splits[11], (EXPERTS, D, FF), (D // 9) ** -0.5, 0.375, ((0, 8), (2, 4)))
    up_weight = gaussian(splits[12], (EXPERTS, D, FF), (D // 9) ** -0.5, 0.375, ((0, 8), (2, 4)))
    down_weight = gaussian(splits[13], (EXPERTS, FF, D), (16 * FF) ** -0.5, 0.03125, ((0, 8), (2, 4)))
    return {"mixer_input": mixer_input, "mixer_gain": mixer_gain, "query_weight": query_weight, "key_weight": key_weight, "value_weight": value_weight, "output_weight": output_weight, "sink_logit": sink_logit, "expert_input": expert_input, "expert_gain": expert_gain, "routes": routes, "route_logits": route_logits, "gate_weight": gate_weight, "up_weight": up_weight, "down_weight": down_weight}


EPSILON = 1e-06
LIMIT = 7.0
SLOPE = 1.702
BASE = 10000.0

def normalize(rows, gain):
    values = rows.astype(jnp.float32)
    scaled = values * lax.rsqrt(lax.optimization_barrier(jnp.mean(values * values, axis=-1, keepdims=True)) + EPSILON)
    return (scaled * gain).astype(jnp.bfloat16)

def turn(values, cosine, sine):
    first, second = jnp.split(values, 2, axis=-1)
    cosine = cosine[:, None, :]
    sine = sine[:, None, :]
    return jnp.concatenate([first * cosine - second * sine, second * cosine + first * sine], axis=-1)

def axial_rope(values, places):
    quarter = values.shape[-1] // 4
    frequency = BASE ** (-jnp.arange(quarter, dtype=jnp.float32) / quarter)
    row_angle = (places // GRID_W).astype(jnp.float32)[:, None] * frequency[None, :]
    column_angle = (places % GRID_W).astype(jnp.float32)[:, None] * frequency[None, :]
    row_part, column_part = jnp.split(values, 2, axis=-1)
    return jnp.concatenate([turn(row_part, jnp.cos(row_angle), jnp.sin(row_angle)), turn(column_part, jnp.cos(column_angle), jnp.sin(column_angle))], axis=-1)

def activate(gate, up):
    capped = jnp.minimum(gate, LIMIT)
    bounded = jnp.clip(up, -LIMIT, LIMIT)
    return (capped * jax.nn.sigmoid(SLOPE * capped) * (bounded + 1.0)).astype(jnp.bfloat16)

def band_attention(parts):
    query, keys, values, sinks = parts
    total = query.shape[0]
    group = query.shape[1]
    blocks = total // WINDOW
    padded_keys = jnp.pad(keys, ((WINDOW, WINDOW), (0, 0))).reshape(blocks + 2, WINDOW, HEAD_DIM)
    padded_values = jnp.pad(values, ((WINDOW, WINDOW), (0, 0))).reshape(blocks + 2, WINDOW, HEAD_DIM)
    near_keys = jnp.concatenate([padded_keys[:-2], padded_keys[1:-1], padded_keys[2:]], axis=1)
    near_values = jnp.concatenate([padded_values[:-2], padded_values[1:-1], padded_values[2:]], axis=1)
    blocked = query.reshape(blocks, WINDOW, group, HEAD_DIM)
    scores = jnp.einsum('nqrd,nkd->nrqk', blocked.astype(jnp.float32), near_keys.astype(jnp.float32)) * HEAD_DIM ** (-0.5)
    query_place = jnp.arange(total, dtype=jnp.int32).reshape(blocks, WINDOW)
    key_place = (jnp.arange(blocks, dtype=jnp.int32)[:, None] - 1) * WINDOW + jnp.arange(3 * WINDOW, dtype=jnp.int32)[None, :]
    allowed = (jnp.abs(query_place[:, :, None] - key_place[:, None, :]) <= WINDOW) & (key_place[:, None, :] >= 0) & (key_place[:, None, :] < total)
    scores = jnp.where(allowed[:, None], scores, -1e+30)
    sink_column = sinks[None, :, None]
    top = jnp.maximum(lax.optimization_barrier(jnp.max(scores, axis=-1)), sink_column)
    weights = jnp.exp(scores - top[..., None])
    denominator = lax.optimization_barrier(jnp.sum(weights, axis=-1)) + jnp.exp(sink_column - top)
    shares = (weights / denominator[..., None]).astype(jnp.bfloat16)
    mixed = jnp.einsum('nrqk,nkd->nqrd', shares.astype(jnp.float32), near_values.astype(jnp.float32))
    return mixed.astype(jnp.bfloat16).reshape(total, group * HEAD_DIM)

def mixer_half(mixer_input, mixer_gain, query_weight, key_weight, value_weight, output_weight, sink_logit):
    total = mixer_input.shape[0]
    group = HEADS // KV_HEADS
    normed = normalize(mixer_input, mixer_gain)
    places = jnp.arange(total, dtype=jnp.int32)
    query = jnp.dot(normed, query_weight, preferred_element_type=jnp.float32).reshape(total, HEADS, HEAD_DIM)
    query = axial_rope(query, places).astype(jnp.bfloat16).reshape(total, KV_HEADS, group, HEAD_DIM)
    keys = jnp.dot(normed, key_weight, preferred_element_type=jnp.float32).reshape(total, KV_HEADS, HEAD_DIM)
    keys = axial_rope(keys, places).astype(jnp.bfloat16)
    values = jnp.dot(normed, value_weight, preferred_element_type=jnp.float32).astype(jnp.bfloat16).reshape(total, KV_HEADS, HEAD_DIM)
    mixed = lax.map(band_attention, (query.transpose(1, 0, 2, 3), keys.transpose(1, 0, 2), values.transpose(1, 0, 2), sink_logit.reshape(KV_HEADS, group)))
    mixed = mixed.transpose(1, 0, 2).reshape(total, HEADS * HEAD_DIM)
    return jnp.dot(mixed, output_weight, preferred_element_type=jnp.float32).astype(jnp.bfloat16)

def expert_half(expert_input, expert_gain, routes, route_logits, gate_weight, up_weight, down_weight):
    normed = normalize(expert_input, expert_gain)
    chances = jax.nn.softmax(route_logits, axis=-1)
    chosen = routes.reshape(-1)
    count = chosen.shape[0]
    marks = (chosen[:, None] == jnp.arange(EXPERTS, dtype=jnp.int32)[None, :]).astype(jnp.int32)
    earlier = lax.optimization_barrier(jnp.sum((jnp.cumsum(marks, axis=0) - marks) * marks, axis=1))
    room = N_EP * CAP
    target = chosen * room + earlier
    holder = jnp.full((EXPERTS * room,), count, jnp.int32).at[target].set(jnp.arange(count, dtype=jnp.int32))
    holder = (holder // TOP_K).reshape(EXPERTS, room)
    padded = jnp.concatenate([normed, jnp.zeros((1, normed.shape[1]), jnp.bfloat16)], axis=0)

    def serve(parts):
        token_index, gate_part, up_part, down_part = parts
        rows = padded[token_index]
        gate = jnp.dot(rows, gate_part, preferred_element_type=jnp.float32)
        up = jnp.dot(rows, up_part, preferred_element_type=jnp.float32)
        hidden = activate(gate, up)
        return jnp.dot(hidden, down_part, preferred_element_type=jnp.float32).astype(jnp.bfloat16)
    served = lax.map(serve, (holder, gate_weight, up_weight, down_weight))
    flat = served.reshape(EXPERTS * room, served.shape[2])
    picked = flat[target].astype(jnp.float32).reshape(-1, TOP_K, served.shape[2])
    return lax.optimization_barrier(jnp.sum(picked * chances[:, :, None], axis=1)).astype(jnp.bfloat16)

def reference(mixer_input, mixer_gain, query_weight, key_weight, value_weight, output_weight, sink_logit, expert_input, expert_gain, routes, route_logits, gate_weight, up_weight, down_weight):
    mixer_output = mixer_half(mixer_input, mixer_gain, query_weight, key_weight, value_weight, output_weight, sink_logit)
    expert_output = expert_half(expert_input, expert_gain, routes, route_logits, gate_weight, up_weight, down_weight)
    return (mixer_output, expert_output)
```

```python
import functools

import jax
import jax.numpy as jnp
from jax import lax
from jax.experimental import pallas as pl
from jax.experimental.pallas import tpu as pltpu
from jax.sharding import PartitionSpec as P

HEAD_DIM = 64
TOP_K = 4
WINDOW = 128
GRID_W = 64


EPSILON = 1e-06
LIMIT = 7.0
SLOPE = 1.702
BASE = 10000.0


def extended(shard, sides, width):
    for axis, dim in sides:
        devices, length = (lax.axis_size(axis), shard.shape[dim])
        up = [(i, (i + 1) % devices) for i in range(devices - 1)]
        down = [(j, i) for i, j in up]
        last = lax.slice_in_dim(shard, length - width, length, axis=dim)
        first = lax.slice_in_dim(shard, 0, width, axis=dim)
        before = lax.ppermute(last, axis, up)
        after = lax.ppermute(first, axis, down)
        shard = jnp.concatenate([before, shard, after], axis=dim)
    return shard


def normalize(rows, gain):
    values = rows.astype(jnp.float32)
    scaled = values * lax.rsqrt(jnp.mean(values * values, axis=-1, keepdims=True) + EPSILON)
    return (scaled * gain).astype(jnp.bfloat16)


def turn(values, cosine, sine):
    first, second = jnp.split(values, 2, axis=-1)
    cosine = cosine[:, None, :]
    sine = sine[:, None, :]
    return jnp.concatenate(
        [first * cosine - second * sine, second * cosine + first * sine], axis=-1
    )


def axial_rope(values, places):
    quarter = values.shape[-1] // 4
    frequency = BASE ** (-jnp.arange(quarter, dtype=jnp.float32) / quarter)
    row_angle = (places // GRID_W).astype(jnp.float32)[:, None] * frequency[None, :]
    column_angle = (places % GRID_W).astype(jnp.float32)[:, None] * frequency[None, :]
    row_part, column_part = jnp.split(values, 2, axis=-1)
    return jnp.concatenate(
        [
            turn(row_part, jnp.cos(row_angle), jnp.sin(row_angle)),
            turn(column_part, jnp.cos(column_angle), jnp.sin(column_angle)),
        ],
        axis=-1,
    )


def activate(gate, up):
    capped = jnp.minimum(gate, LIMIT)
    bounded = jnp.clip(up, -LIMIT, LIMIT)
    return (capped * jax.nn.sigmoid(SLOPE * capped) * (bounded + 1.0)).astype(jnp.bfloat16)


def remote(src, dst, sent, landed, ep, tp):
    return pltpu.make_async_remote_copy(
        src_ref=src,
        dst_ref=dst,
        send_sem=sent,
        recv_sem=landed,
        device_id=(ep, tp),
        device_id_type=pl.DeviceIdType.MESH,
    )


def exchange(
    n,
    t,
    x_ref,
    gain_ref,
    share_ref,
    mixed_ref,
    wo_hbm,
    wg_hbm,
    wu_hbm,
    wd_hbm,
    mixer_out,
    expert_out,
    tokens,
    hidden,
    heads,
    result,
    returned,
    wo,
    wg,
    wu,
    wd,
    local_sem,
    token_recv,
    far_send,
    near_send,
    core_send,
    hidden_send,
    hidden_recv,
    head_send,
    head_recv,
    result_send,
    result_recv,
):
    ep, tp = lax.axis_index("ep"), lax.axis_index("tp")
    chips = n // 2
    z, core = ep // 2, ep % 2
    step = 1 - 2 * core
    partner = 2 * z + 1 - core
    rows = x_ref.shape[0]
    pair = 2 * rows
    part = wg.shape[1]
    far, near = chips // 2, chips - 1 - chips // 2

    def chip(hops):
        return lax.rem(z + hops * step + 2 * chips, chips)

    def block(buffer, index, size):
        return buffer.at[pl.ds(pl.multiple_of(index * size, size), size)]

    loads = [
        pltpu.make_async_copy(a, b, local_sem.at[i])
        for i, (a, b) in enumerate(((wg_hbm, wg), (wu_hbm, wu), (wo_hbm, wo), (wd_hbm, wd)))
    ]
    for load in loads:
        load.start()

    barrier = pltpu.get_barrier_semaphore()
    for k in range(1, n):
        pl.semaphore_signal(
            barrier,
            inc=1,
            device_id=(lax.rem(ep + k, n), tp),
            device_id_type=pl.DeviceIdType.MESH,
        )
    for k in range(1, t):
        pl.semaphore_signal(
            barrier,
            inc=1,
            device_id=(ep, lax.rem(tp + k, t)),
            device_id_type=pl.DeviceIdType.MESH,
        )
    tokens[pl.ds(pl.multiple_of(ep * rows, rows), rows), :] = normalize(x_ref[...], gain_ref[...])
    pl.semaphore_wait(barrier, n + t - 2)

    def token_copy(slot, sent, target):
        piece = block(tokens, slot, rows)
        return remote(piece, piece, sent, token_recv.at[slot], target, tp)

    def forward_far(hop):
        return token_copy(2 * chip(-hop) + core, far_send.at[hop], 2 * chip(1) + core)

    def forward_near(hop):
        return token_copy(2 * chip(hop) + core, near_send.at[hop], 2 * chip(-1) + core)

    def forward_core(hops):
        place = chip(hops)
        return token_copy(2 * place + core, core_send.at[place], partner)

    def token_wait(slot):
        token_copy(slot, core_send.at[0], partner).wait_recv()

    if far > 0:
        forward_far(0).start()
    if near > 0:
        forward_near(0).start()
    forward_core(0).start()

    def head_copy(source, k):
        return remote(
            mixed_ref, heads.at[source], head_send.at[k], head_recv.at[source], ep, lax.rem(tp + k, t)
        )

    for k in range(1, t):
        head_copy(tp, k).start()
    heads[tp] = mixed_ref[...]

    def hidden_copy(source, place, k):
        piece = block(hidden.at[source], place, pair)
        return remote(
            piece,
            piece,
            hidden_send.at[k, place],
            hidden_recv.at[source, place],
            ep,
            lax.rem(tp + k, t),
        )

    def first_half(place):
        token_wait(2 * place + 1 - core)
        inside = pl.ds(pl.multiple_of(place * pair, pair), pair)
        span = min(256, part)
        for start in range(0, part, span):
            cut = slice(start, start + span)
            gate = jnp.dot(tokens[inside, :], wg[:, cut], preferred_element_type=jnp.float32)
            up = jnp.dot(tokens[inside, :], wu[:, cut], preferred_element_type=jnp.float32)
            hidden[tp, inside, cut] = activate(gate, up)
        for k in range(1, t):
            hidden_copy(tp, place, k).start()

    loads[0].wait()
    loads[1].wait()
    first_half(z)
    for hop in range(1, far + 1):
        token_wait(2 * chip(-hop) + core)
        if hop < far:
            forward_far(hop).start()
        forward_core(-hop).start()
        if hop <= near:
            token_wait(2 * chip(hop) + core)
            if hop < near:
                forward_near(hop).start()
            forward_core(hop).start()

            def both(k, carry, hop=hop):
                first_half(chip((2 * k - 1) * hop))
                return carry

            lax.fori_loop(0, 2, both, 0)
        else:
            first_half(chip(-hop))

    loads[2].wait()
    for k in range(1, t):
        head_copy(lax.rem(tp + k, t), k).wait_recv()
    total = jnp.dot(heads[0], wo[0:part, :], preferred_element_type=jnp.float32)
    for k in range(1, t):
        total += jnp.dot(
            heads[k], wo[k * part : (k + 1) * part, :], preferred_element_type=jnp.float32
        )
    mixer_out[...] = total.astype(jnp.bfloat16)

    loads[3].wait()

    def result_copy(source, owner):
        return remote(
            block(result, owner, rows),
            returned.at[source],
            result_send.at[owner],
            result_recv.at[source],
            owner,
            tp,
        )

    def second_half(i, carry):
        hop = (i + 1) // 2
        place = chip(hop * (2 * ((i + 1) % 2) - 1))
        inside = pl.ds(pl.multiple_of(place * pair, pair), pair)
        for k in range(1, t):
            hidden_copy(lax.rem(tp + k, t), place, k).wait_recv()
        total = jnp.dot(hidden[0, inside, :], wd[0:part, :], preferred_element_type=jnp.float32)
        for k in range(1, t):
            total += jnp.dot(
                hidden[k, inside, :],
                wd[k * part : (k + 1) * part, :],
                preferred_element_type=jnp.float32,
            )
        result[inside, :] = total.astype(jnp.bfloat16)

        @pl.when(i == 0)
        def _():
            result_copy(ep, partner).start()
            returned[ep] = result[pl.ds(pl.multiple_of(ep * rows, rows), rows), :]

        @pl.when(i > 0)
        def _():
            result_copy(ep, 2 * place + core).start()
            result_copy(ep, 2 * place + 1 - core).start()

        return carry

    lax.fori_loop(0, chips, second_half, 0)

    for k in range(1, n):
        other = lax.rem(ep + k, n)
        result_copy(other, other).wait_recv()
    total = returned[0].astype(jnp.float32) * share_ref[:, 0:1]
    for e in range(1, n):
        total += returned[e].astype(jnp.float32) * share_ref[:, e : e + 1]
    expert_out[...] = total.astype(jnp.bfloat16)

    for hop in range(far):
        forward_far(hop).wait_send()
    for hop in range(near):
        forward_near(hop).wait_send()
    for hop in range(chips):
        forward_core(hop).wait_send()
    for k in range(1, t):
        head_copy(tp, k).wait_send()
        for place in range(chips):
            hidden_copy(tp, place, k).wait_send()
    for k in range(1, n):
        result_copy(ep, lax.rem(ep + k, n)).wait_send()


def shards(
    mixer_input,
    mixer_gain,
    query_weight,
    key_weight,
    value_weight,
    output_weight,
    sink_logit,
    expert_input,
    expert_gain,
    routes,
    route_logits,
    gate_weight,
    up_weight,
    down_weight,
):
    tokens = mixer_input.shape[0]
    query_heads = query_weight.shape[1] // HEAD_DIM
    key_heads = key_weight.shape[1] // HEAD_DIM
    group = query_heads // key_heads
    blocks = tokens // WINDOW
    offset = lax.axis_index("ep") * tokens
    length = lax.axis_size("ep") * tokens
    places = offset + jnp.arange(tokens, dtype=jnp.int32)
    normed = normalize(mixer_input, mixer_gain)
    query = jnp.dot(normed, query_weight, preferred_element_type=jnp.float32).reshape(
        tokens, query_heads, HEAD_DIM
    )
    query = (
        axial_rope(query, places)
        .astype(jnp.bfloat16)
        .reshape(blocks, WINDOW, key_heads, group, HEAD_DIM)
    )
    keys = jnp.dot(normed, key_weight, preferred_element_type=jnp.float32).reshape(
        tokens, key_heads, HEAD_DIM
    )
    keys = axial_rope(keys, places).astype(jnp.bfloat16).reshape(tokens, key_heads * HEAD_DIM)
    values = jnp.dot(normed, value_weight, preferred_element_type=jnp.float32).astype(jnp.bfloat16)
    stacked = jnp.concatenate([keys, values], axis=1)
    widened = extended(stacked, (("ep", 0),), WINDOW)
    framed = widened.reshape(blocks + 2, WINDOW, 2, key_heads, HEAD_DIM)
    nearby = jnp.concatenate([framed[:-2], framed[1:-1], framed[2:]], axis=1)
    scores = jnp.einsum(
        "nqgrd,nkgd->ngrqk", query, nearby[:, :, 0], preferred_element_type=jnp.float32
    ) * HEAD_DIM ** (-0.5)
    query_place = places.reshape(blocks, WINDOW)
    key_place = (
        offset
        + (jnp.arange(blocks, dtype=jnp.int32)[:, None] - 1) * WINDOW
        + jnp.arange(3 * WINDOW, dtype=jnp.int32)[None, :]
    )
    allowed = (
        (jnp.abs(query_place[:, :, None] - key_place[:, None, :]) <= WINDOW)
        & (key_place[:, None, :] >= 0)
        & (key_place[:, None, :] < length)
    )
    scores = jnp.where(allowed[:, None, None], scores, -1e30)
    sinks = sink_logit.reshape(key_heads, group)[None, :, :, None]
    top = jnp.maximum(jnp.max(scores, axis=-1), sinks)
    weights = jnp.exp(scores - top[..., None])
    denominator = jnp.sum(weights, axis=-1) + jnp.exp(sinks - top)
    shares = (weights / denominator[..., None]).astype(jnp.bfloat16)
    mixed = jnp.einsum(
        "ngrqk,nkgd->nqgrd", shares, nearby[:, :, 1], preferred_element_type=jnp.float32
    )
    mixed = mixed.astype(jnp.bfloat16).reshape(tokens, query_heads * HEAD_DIM)
    experts = lax.axis_size("ep")
    parts = lax.axis_size("tp")
    rows_here, width = expert_input.shape
    part = gate_weight.shape[2]
    chances = jax.nn.softmax(route_logits, axis=-1)
    named = routes[:, :, None] == jnp.arange(experts, dtype=jnp.int32)[None, None, :]
    expert_share = jnp.sum(jnp.where(named, chances[:, :, None], 0.0), axis=1)
    vmem = pl.BlockSpec(memory_space=pltpu.VMEM)
    anywhere = pl.BlockSpec(memory_space=pl.ANY)
    chips = experts // 2
    dma = pltpu.SemaphoreType.DMA
    columns = down_weight.shape[2]
    return pl.pallas_call(
        functools.partial(exchange, experts, parts),
        out_shape=(
            jax.ShapeDtypeStruct((tokens, output_weight.shape[1]), jnp.bfloat16),
            jax.ShapeDtypeStruct((rows_here, columns), jnp.bfloat16),
        ),
        in_specs=[vmem] * 4 + [anywhere] * 4,
        out_specs=(vmem, vmem),
        scratch_shapes=[
            pltpu.VMEM((experts * rows_here, width), jnp.bfloat16),
            pltpu.VMEM((parts, experts * rows_here, part), jnp.bfloat16),
            pltpu.VMEM((parts, tokens, mixed.shape[1]), jnp.bfloat16),
            pltpu.VMEM((experts * rows_here, columns), jnp.bfloat16),
            pltpu.VMEM((experts, rows_here, columns), jnp.bfloat16),
            pltpu.VMEM(output_weight.shape, jnp.bfloat16),
            pltpu.VMEM(gate_weight.shape[1:], jnp.bfloat16),
            pltpu.VMEM(up_weight.shape[1:], jnp.bfloat16),
            pltpu.VMEM(down_weight.shape[1:], jnp.bfloat16),
            dma((4,)),
            dma((experts,)),
            dma((chips,)),
            dma((chips,)),
            dma((chips,)),
            dma((parts, chips)),
            dma((parts, chips)),
            dma((parts,)),
            dma((parts,)),
            dma((experts,)),
            dma((experts,)),
        ],
        compiler_params=pltpu.CompilerParams(
            collective_id=0, has_side_effects=True, vmem_limit_bytes=60 * 1024 * 1024
        ),
    )(
        expert_input,
        expert_gain.reshape(1, -1),
        expert_share,
        mixed,
        output_weight,
        gate_weight[0],
        up_weight[0],
        down_weight[0],
    )


def solution(mesh):
    return jax.shard_map(
        shards,
        mesh=mesh,
        in_specs=(
            P("ep", None),
            P(),
            P(None, "tp"),
            P(None, "tp"),
            P(None, "tp"),
            P(None, "tp"),
            P("tp"),
            P("ep", None),
            P(),
            P("ep", None),
            P("ep", None),
            P("ep", None, "tp"),
            P("ep", None, "tp"),
            P("ep", None, "tp"),
        ),
        out_specs=(P("ep", "tp"), P("ep", "tp")),
        check_vma=False,
    )
```

```python
import functools

import jax
import jax.numpy as jnp
from jax import lax
from jax.experimental import pallas as pl
from jax.experimental.pallas import tpu as pltpu
from jax.sharding import PartitionSpec as P

HEAD_DIM = 64
TOP_K = 4
WINDOW = 128
GRID_W = 64


EPSILON = 1e-06
LIMIT = 7.0
SLOPE = 1.702
BASE = 10000.0


def normalize(rows, gain):
    values = rows.astype(jnp.float32)
    scaled = values * lax.rsqrt(jnp.mean(values * values, axis=-1, keepdims=True) + EPSILON)
    return (scaled * gain).astype(jnp.bfloat16)


def rotate(values, cosine, sine):
    width = values.shape[1]
    lanes = cosine.shape[1]
    if width < lanes:
        return rotate(jnp.concatenate([values] * (lanes // width), axis=1), cosine, sine)[:, :width]
    spot = lax.broadcasted_iota(jnp.int32, cosine.shape, 1)
    leading = spot % (HEAD_DIM // 2) < HEAD_DIM // 4
    pieces = []
    for start in range(0, width, lanes):
        piece = values[:, start : start + lanes]
        other = jnp.where(
            leading,
            pltpu.roll(piece, lanes - HEAD_DIM // 4, 1),
            pltpu.roll(piece, HEAD_DIM // 4, 1),
        )
        pieces.append(piece * cosine + other * sine)
    return jnp.concatenate(pieces, axis=1)


def activate(gate, up):
    capped = jnp.minimum(gate, LIMIT)
    bounded = jnp.clip(up, -LIMIT, LIMIT)
    return (capped * jax.nn.sigmoid(SLOPE * capped) * (bounded + 1.0)).astype(jnp.bfloat16)


def remote(src, dst, sent, landed, ep, tp):
    return pltpu.make_async_remote_copy(
        src_ref=src,
        dst_ref=dst,
        send_sem=sent,
        recv_sem=landed,
        device_id=(ep, tp),
        device_id_type=pl.DeviceIdType.MESH,
    )


def exchange(
    n,
    t,
    x_ref,
    gain_ref,
    share_ref,
    mixer_ref,
    mixer_gain_ref,
    cosine_ref,
    sine_ref,
    sink_ref,
    wq_hbm,
    wk_hbm,
    wv_hbm,
    wo_hbm,
    wg_hbm,
    wu_hbm,
    wd_hbm,
    mixer_out,
    expert_out,
    tokens,
    hidden,
    heads,
    result,
    returned,
    queries,
    around,
    wq,
    wk,
    wv,
    wo,
    wg,
    wu,
    wd,
    local_sem,
    token_recv,
    far_send,
    near_send,
    core_send,
    hidden_send,
    hidden_recv,
    pass_send,
    pass_recv,
    head_send,
    head_recv,
    edge_send,
    edge_recv,
    result_send,
    result_recv,
):
    ep, tp = lax.axis_index("ep"), lax.axis_index("tp")
    chips = n // 2
    z, core = ep // 2, ep % 2
    step = 1 - 2 * core
    partner = 2 * z + 1 - core
    rows = x_ref.shape[0]
    pair = 2 * rows
    part = wg.shape[1]
    far, near = chips // 2, chips - 1 - chips // 2
    square = t == 4
    direct = (1, 2) if square else tuple(range(1, t))

    def peer(k):
        if not square:
            return lax.rem(tp + k, t)
        return lax.rem(tp + (k // 2) * 2 + (k % 2) * (1 - 2 * (tp % 2)) + t, t)

    def chip(hops):
        return lax.rem(z + hops * step + 2 * chips, chips)

    def block(buffer, index, size):
        return buffer.at[pl.ds(pl.multiple_of(index * size, size), size)]

    loads = [
        pltpu.make_async_copy(a, b, local_sem.at[i])
        for i, (a, b) in enumerate((
            (wq_hbm, wq),
            (wk_hbm, wk),
            (wv_hbm, wv),
            (wg_hbm, wg),
            (wu_hbm, wu),
            (wo_hbm, wo),
            (wd_hbm, wd),
        ))
    ]
    for load in loads:
        load.start()

    barrier = pltpu.get_barrier_semaphore()
    for k in range(1, n):
        pl.semaphore_signal(
            barrier,
            inc=1,
            device_id=(lax.rem(ep + k, n), tp),
            device_id_type=pl.DeviceIdType.MESH,
        )
    for k in range(1, t):
        pl.semaphore_signal(
            barrier,
            inc=1,
            device_id=(ep, peer(k)),
            device_id_type=pl.DeviceIdType.MESH,
        )
    tokens[pl.ds(pl.multiple_of(ep * rows, rows), rows), :] = normalize(x_ref[...], gain_ref[...])
    pl.semaphore_wait(barrier, n + t - 2)

    def token_copy(slot, sent, target):
        piece = block(tokens, slot, rows)
        return remote(piece, piece, sent, token_recv.at[slot], target, tp)

    def forward_far(hop):
        return token_copy(2 * chip(-hop) + core, far_send.at[hop], 2 * chip(1) + core)

    def forward_near(hop):
        return token_copy(2 * chip(hop) + core, near_send.at[hop], 2 * chip(-1) + core)

    def forward_core(hops):
        place = chip(hops)
        return token_copy(2 * place + core, core_send.at[place], partner)

    def token_wait(slot):
        token_copy(slot, core_send.at[0], partner).wait_recv()

    if far > 0:
        forward_far(0).start()
    if near > 0:
        forward_near(0).start()
    forward_core(0).start()

    def head_copy(source, k):
        piece = heads.at[source]
        return remote(piece, piece, head_send.at[k], head_recv.at[source], ep, peer(k))

    def pass_copy(place, way):
        source = peer(2 - way)
        if place is None:
            start, size, index = 0, heads.shape[1] // 2, chips
            buffer = heads.at[source]
        else:
            start, size, index = place * pair, rows, place
            buffer = hidden.at[source]
        piece = buffer.at[pl.ds(pl.multiple_of(start + (1 - way) * size, size), size)]
        return remote(
            piece, piece, pass_send.at[way, index], pass_recv.at[way, index], ep, peer(1 + way)
        )

    def pass_wait(place, way):
        if place is None:
            start, size, index = 0, heads.shape[1] // 2, chips
            buffer = heads.at[peer(3)]
        else:
            start, size, index = place * pair, rows, place
            buffer = hidden.at[peer(3)]
        piece = buffer.at[pl.ds(pl.multiple_of(start + (1 - way) * size, size), size)]
        remote(
            piece, piece, pass_send.at[way, index], pass_recv.at[way, index], ep, peer(1 + way)
        ).wait_recv()

    def hidden_copy(source, place, k):
        piece = block(hidden.at[source], place, pair)
        return remote(
            piece,
            piece,
            hidden_send.at[k, place],
            hidden_recv.at[source, place],
            ep,
            peer(k),
        )

    def hidden_pass(place):
        if square:
            for way in range(2):
                hidden_copy(peer(2 - way), place, 2 - way).wait_recv()
                pass_copy(place, way).start()

    def hidden_wait(place):
        if square:
            for way in range(2):
                pass_wait(place, way)
        else:
            for k in direct:
                hidden_copy(peer(k), place, k).wait_recv()

    def first_half(place):
        token_wait(2 * place + 1 - core)
        inside = pl.ds(pl.multiple_of(place * pair, pair), pair)
        span = min(256, part)
        for start in range(0, part, span):
            cut = slice(start, start + span)
            gate = jnp.dot(tokens[inside, :], wg[:, cut], preferred_element_type=jnp.float32)
            up = jnp.dot(tokens[inside, :], wu[:, cut], preferred_element_type=jnp.float32)
            hidden[tp, inside, cut] = activate(gate, up)
        for k in direct:
            hidden_copy(tp, place, k).start()

    length = mixer_ref.shape[0]
    kept = wk.shape[1]
    normed = normalize(mixer_ref[...], mixer_gain_ref[...])
    cosine, sine = cosine_ref[...], sine_ref[...]
    own = slice(WINDOW, WINDOW + length)
    for load in loads[:3]:
        load.wait()
    keys = jnp.dot(normed, wk[...], preferred_element_type=jnp.float32)
    around[own, 0:kept] = rotate(keys, cosine, sine).astype(jnp.bfloat16)
    around[own, kept:] = jnp.dot(normed, wv[...], preferred_element_type=jnp.float32).astype(
        jnp.bfloat16
    )

    def edge_copy(way):
        source, target = (length, 0) if way == 0 else (WINDOW, WINDOW + length)
        return remote(
            around.at[pl.ds(source, WINDOW)],
            around.at[pl.ds(target, WINDOW)],
            edge_send.at[way],
            edge_recv.at[way],
            lax.rem(ep + (1 if way == 0 else n - 1), n),
            tp,
        )

    for way in range(2):
        edge_copy(way).start()
    turned = jnp.dot(normed, wq[...], preferred_element_type=jnp.float32)
    queries[...] = rotate(turned, cosine, sine).astype(jnp.bfloat16)

    loads[3].wait()
    loads[4].wait()
    first_half(z)

    def attend(number, carry):
        inside = pl.ds(pl.multiple_of(number * WINDOW, WINDOW), WINDOW)
        seen = pl.ds(pl.multiple_of(number * WINDOW, WINDOW), 3 * WINDOW)
        shape = (WINDOW, 3 * WINDOW)
        line = lax.broadcasted_iota(jnp.int32, shape, 0)
        key = lax.broadcasted_iota(jnp.int32, shape, 1)
        place = ep * length + (number - 1) * WINDOW + key
        allowed = (key >= line) & (key <= line + 2 * WINDOW) & (place >= 0) & (place < n * length)
        group = queries.shape[1] // kept
        allowed = jnp.concatenate([allowed] * group, axis=0)
        for head in range(kept // HEAD_DIM):
            first = head * group
            query = jnp.concatenate(
                [
                    queries[inside, (first + r) * HEAD_DIM : (first + r + 1) * HEAD_DIM]
                    for r in range(group)
                ],
                axis=0,
            )
            sinks = jnp.concatenate(
                [
                    jnp.broadcast_to(sink_ref[:, first + r : first + r + 1], (WINDOW, 1))
                    for r in range(group)
                ],
                axis=0,
            )
            near_keys = around[seen, head * HEAD_DIM : (head + 1) * HEAD_DIM]
            near_values = around[seen, kept + head * HEAD_DIM : kept + (head + 1) * HEAD_DIM]
            scores = lax.dot_general(
                query,
                near_keys,
                (((1,), (1,)), ((), ())),
                preferred_element_type=jnp.float32,
            ) * HEAD_DIM ** (-0.5)
            scores = jnp.where(allowed, scores, -1e30)
            top = jnp.maximum(jnp.max(scores, axis=-1, keepdims=True), sinks)
            weights = jnp.exp(scores - top)
            denominator = jnp.sum(weights, axis=-1, keepdims=True) + jnp.exp(sinks - top)
            shares = (weights * (1.0 / denominator)).astype(jnp.bfloat16)
            mixed = jnp.dot(shares, near_values, preferred_element_type=jnp.float32)
            mixed = mixed.astype(jnp.bfloat16)
            heads[tp, inside, first * HEAD_DIM : (first + group) * HEAD_DIM] = jnp.concatenate(
                [mixed[r * WINDOW : (r + 1) * WINDOW] for r in range(group)], axis=1
            )
        return carry

    def attention():
        for way in range(2):
            edge_copy(way).wait_recv()
        lax.fori_loop(0, length // WINDOW, attend, 0)
        for k in direct:
            head_copy(tp, k).start()

    for hop in range(1, far + 1):
        token_wait(2 * chip(-hop) + core)
        if hop < far:
            forward_far(hop).start()
        forward_core(-hop).start()
        if hop <= near:
            token_wait(2 * chip(hop) + core)
            if hop < near:
                forward_near(hop).start()
            forward_core(hop).start()
            if hop == 1:
                attention()

            def both(k, carry, hop=hop):
                first_half(chip((2 * k - 1) * hop))
                return carry

            lax.fori_loop(0, 2, both, 0)
            if hop == 1 and square:
                hidden_pass(z)
                for way in range(2):
                    head_copy(peer(2 - way), 2 - way).wait_recv()
                    pass_copy(None, way).start()
        else:
            first_half(chip(-hop))

    def place_of(i):
        return chip((i + 1) // 2 * (2 * ((i + 1) % 2) - 1))

    def pass_on(i, carry):
        hidden_pass(place_of(i))
        return carry

    lax.fori_loop(1, chips - 1, pass_on, 0)

    loads[5].wait()
    if square:
        for way in range(2):
            pass_wait(None, way)
    else:
        for k in direct:
            head_copy(peer(k), k).wait_recv()
    total = jnp.dot(heads[0], wo[0:part, :], preferred_element_type=jnp.float32)
    for k in range(1, t):
        total += jnp.dot(
            heads[k], wo[k * part : (k + 1) * part, :], preferred_element_type=jnp.float32
        )
    mixer_out[...] = total.astype(jnp.bfloat16)

    loads[6].wait()

    def result_copy(source, owner):
        return remote(
            block(result, owner, rows),
            returned.at[source],
            result_send.at[owner],
            result_recv.at[source],
            owner,
            tp,
        )

    def second_half(i, carry):
        place = place_of(i)
        inside = pl.ds(pl.multiple_of(place * pair, pair), pair)
        hidden_wait(place)
        total = jnp.dot(hidden[0, inside, :], wd[0:part, :], preferred_element_type=jnp.float32)
        for k in range(1, t):
            total += jnp.dot(
                hidden[k, inside, :],
                wd[k * part : (k + 1) * part, :],
                preferred_element_type=jnp.float32,
            )
        result[inside, :] = total.astype(jnp.bfloat16)

        @pl.when(i == 0)
        def _():
            result_copy(ep, partner).start()
            returned[ep] = result[pl.ds(pl.multiple_of(ep * rows, rows), rows), :]

        @pl.when(i > 0)
        def _():
            result_copy(ep, 2 * place + core).start()
            result_copy(ep, 2 * place + 1 - core).start()

        return carry

    lax.fori_loop(0, chips - 2, second_half, 0)
    hidden_pass(place_of(chips - 1))
    lax.fori_loop(chips - 2, chips, second_half, 0)

    for k in range(1, n):
        other = lax.rem(ep + k, n)
        result_copy(other, other).wait_recv()
    total = returned[0].astype(jnp.float32) * share_ref[:, 0:1]
    for e in range(1, n):
        total += returned[e].astype(jnp.float32) * share_ref[:, e : e + 1]
    expert_out[...] = total.astype(jnp.bfloat16)

    for hop in range(far):
        forward_far(hop).wait_send()
    for hop in range(near):
        forward_near(hop).wait_send()
    for hop in range(chips):
        forward_core(hop).wait_send()
    for way in range(2):
        edge_copy(way).wait_send()
        if square:
            pass_copy(None, way).wait_send()
            for place in range(chips):
                pass_copy(place, way).wait_send()
    for k in direct:
        head_copy(tp, k).wait_send()
        for place in range(chips):
            hidden_copy(tp, place, k).wait_send()
    for k in range(1, n):
        result_copy(ep, lax.rem(ep + k, n)).wait_send()


def shards(
    mixer_input,
    mixer_gain,
    query_weight,
    key_weight,
    value_weight,
    output_weight,
    sink_logit,
    expert_input,
    expert_gain,
    routes,
    route_logits,
    gate_weight,
    up_weight,
    down_weight,
):
    tokens = mixer_input.shape[0]
    lanes = 2 * HEAD_DIM
    quarter = HEAD_DIM // 4
    spot = jnp.arange(lanes, dtype=jnp.int32)[None, :]
    place = (lax.axis_index("ep") * tokens + jnp.arange(tokens, dtype=jnp.int32))[:, None]
    frequency = BASE ** (-(spot % quarter).astype(jnp.float32) / quarter)
    by_row = spot % HEAD_DIM < HEAD_DIM // 2
    turn = jnp.where(by_row, place // GRID_W, place % GRID_W).astype(jnp.float32) * frequency
    cosine = jnp.cos(turn)
    sine = jnp.sin(turn) * jnp.where(spot % (HEAD_DIM // 2) < quarter, -1.0, 1.0)
    experts = lax.axis_size("ep")
    parts = lax.axis_size("tp")
    rows_here, width = expert_input.shape
    part = gate_weight.shape[2]
    chances = jax.nn.softmax(route_logits, axis=-1)
    named = routes[:, :, None] == jnp.arange(experts, dtype=jnp.int32)[None, None, :]
    expert_share = jnp.sum(jnp.where(named, chances[:, :, None], 0.0), axis=1)
    vmem = pl.BlockSpec(memory_space=pltpu.VMEM)
    anywhere = pl.BlockSpec(memory_space=pl.ANY)
    chips = experts // 2
    dma = pltpu.SemaphoreType.DMA
    columns = down_weight.shape[2]
    return pl.pallas_call(
        functools.partial(exchange, experts, parts),
        out_shape=(
            jax.ShapeDtypeStruct((tokens, output_weight.shape[1]), jnp.bfloat16),
            jax.ShapeDtypeStruct((rows_here, columns), jnp.bfloat16),
        ),
        in_specs=[vmem] * 8 + [anywhere] * 7,
        out_specs=(vmem, vmem),
        scratch_shapes=[
            pltpu.VMEM((experts * rows_here, width), jnp.bfloat16),
            pltpu.VMEM((parts, experts * rows_here, part), jnp.bfloat16),
            pltpu.VMEM((parts, tokens, query_weight.shape[1]), jnp.bfloat16),
            pltpu.VMEM((experts * rows_here, columns), jnp.bfloat16),
            pltpu.VMEM((experts, rows_here, columns), jnp.bfloat16),
            pltpu.VMEM((tokens, query_weight.shape[1]), jnp.bfloat16),
            pltpu.VMEM((tokens + 2 * WINDOW, 2 * key_weight.shape[1]), jnp.bfloat16),
            pltpu.VMEM(query_weight.shape, jnp.bfloat16),
            pltpu.VMEM(key_weight.shape, jnp.bfloat16),
            pltpu.VMEM(value_weight.shape, jnp.bfloat16),
            pltpu.VMEM(output_weight.shape, jnp.bfloat16),
            pltpu.VMEM(gate_weight.shape[1:], jnp.bfloat16),
            pltpu.VMEM(up_weight.shape[1:], jnp.bfloat16),
            pltpu.VMEM(down_weight.shape[1:], jnp.bfloat16),
            dma((7,)),
            dma((experts,)),
            dma((chips,)),
            dma((chips,)),
            dma((chips,)),
            dma((parts, chips)),
            dma((parts, chips)),
            dma((2, chips + 1)),
            dma((2, chips + 1)),
            dma((parts,)),
            dma((parts,)),
            dma((2,)),
            dma((2,)),
            dma((experts,)),
            dma((experts,)),
        ],
        compiler_params=pltpu.CompilerParams(
            collective_id=0, has_side_effects=True, vmem_limit_bytes=60 * 1024 * 1024
        ),
    )(
        expert_input,
        expert_gain.reshape(1, -1),
        expert_share,
        mixer_input,
        mixer_gain.reshape(1, -1),
        cosine,
        sine,
        sink_logit.reshape(1, -1),
        query_weight,
        key_weight,
        value_weight,
        output_weight,
        gate_weight[0],
        up_weight[0],
        down_weight[0],
    )


def solution(mesh):
    return jax.shard_map(
        shards,
        mesh=mesh,
        in_specs=(
            P("ep", None),
            P(),
            P(None, "tp"),
            P(None, "tp"),
            P(None, "tp"),
            P(None, "tp"),
            P("tp"),
            P("ep", None),
            P(),
            P("ep", None),
            P("ep", None),
            P("ep", None, "tp"),
            P("ep", None, "tp"),
            P("ep", None, "tp"),
        ),
        out_specs=(P("ep", "tp"), P("ep", "tp")),
        check_vma=False,
    )
```
